32 devices in a mesh: sp: 8 (over z, y), tp: 4 (over x, core).
Axes of the slice: x: 2, y: 2, z: 4, core: 2. Of those that a mesh axis runs over, the one named last changes fastest.
Arguments:
- queries: bfloat16 [4096, 1024], P('sp', 'tp'), may hold values from -200 to 200
- keys: bfloat16 [4096, 1024], P('sp', 'tp'), may hold values from -6 to 6
- values: bfloat16 [4096, 1024], P('sp', 'tp'), may hold values from -24 to 24
- cum_gate: float32 [4096, 8], P('sp', 'tp'), may hold values from -414 to 0, as said below
- residual: bfloat16 [4096, 2048], P(('sp', 'tp')), may hold values from -1.5 to 1.5
- w_out: bfloat16 [1024, 2048], replicated, may hold values from -0.1875 to 0.1875
- gain: float32 [2048], replicated, may hold values from 0.1 to 1.9
- w_up: bfloat16 [2048, 8192], P('sp', 'tp'), may hold values from -0.125 to 0.125
- w_down: bfloat16 [8192, 2048], P('tp', 'sp'), may hold values from -0.0625 to 0.0625
Outputs:
- output: bfloat16 [4096, 2048], P(('sp', 'tp'))
The draws below stay inside these ranges and needn't reach their ends.
Inputs may be any that keep to these rules, and one draw needn't show every extreme that they name: Within each head, cum_gate never rises from one position to the next.
All inputs are finite; a program needn't handle non-finite values.
Results may differ from the reference program's by a relative error of at most 0.022.
Values may be sent and summed in bfloat16 or wider, within the bound.
A program may use at most 128 MiB of HBM per device.

```python
import math
import jax
import jax.numpy as jnp
from jax import lax

D = 2048
HEADS = 8
HEAD_DIM = 128
FF = 8192
TOK_DEV = 512
SEQUENCE_TOKENS = 4096
N_TP = 4


def joint_pair(key):
    width = HEADS * HEAD_DIM
    query_key = jax.random.fold_in(key, 101)
    key_key = jax.random.fold_in(key, 202)
    keys = jnp.clip(jax.random.normal(key_key, (SEQUENCE_TOKENS, width), jnp.float32), -6.0, 6.0)
    queries = jnp.clip(2.0 * jax.random.normal(query_key, (SEQUENCE_TOKENS, width), jnp.float32), -12.0, 12.0)
    return (queries, keys)


def draw_queries(key, part):
    return joint_pair(key)[0].astype(jnp.bfloat16)


def draw_keys(key, part):
    return joint_pair(key)[1].astype(jnp.bfloat16)


def draw_cum_gate(key, part):
    shuffle_random_key, gradual_decay_key, quick_decay_key, block_random_key, jitter_random_key, spike_random_key, layer_depth_key = jax.random.split(key, 7)
    order = jax.random.permutation(shuffle_random_key, HEADS)
    slow = order < HEADS // 2
    slow_rate = jax.random.uniform(gradual_decay_key, (HEADS,), jnp.float32, 0.2, 0.6) / SEQUENCE_TOKENS
    fast_rate = 1.0 / jnp.exp(jax.random.uniform(quick_decay_key, (HEADS,), jnp.float32, math.log(30.0), math.log(100.0)))
    rate = jnp.where(slow, slow_rate, fast_rate)
    shards = SEQUENCE_TOKENS // TOK_DEV
    factor = 2.0 ** jax.random.uniform(block_random_key, (shards, HEADS), jnp.float32, -1.0, 1.0)
    token_positions = jnp.arange(SEQUENCE_TOKENS)
    per_row = factor[token_positions // TOK_DEV]
    noise = jax.random.uniform(jitter_random_key, (SEQUENCE_TOKENS, HEADS), jnp.float32, 0.5, 1.5)
    steps = -rate[None, :] * per_row * noise
    spike_events = jax.random.randint(spike_random_key, (3,), 0, SEQUENCE_TOKENS)
    depth = jnp.log(jax.random.uniform(layer_depth_key, (3, HEADS), jnp.float32, 0.6, 0.8))
    match_events = (token_positions[:, None] == spike_events[None, :]).astype(jnp.float32)
    steps = steps + jnp.dot(match_events, depth) * slow.astype(jnp.float32)[None, :]
    return jnp.cumsum(steps, axis=0)


def level_of(own_key, extent, pieces, smallest, top_value):
    level, own = 1.0, jax.random.fold_in(own_key, 6)
    for axis_at, shards_of in pieces:
        heights = jnp.exp(jax.random.uniform(jax.random.fold_in(own, axis_at), (shards_of,), jnp.float32, smallest / len(pieces), top_value / len(pieces)))
        level = level * jnp.repeat(heights, extent[axis_at] // shards_of).reshape([-1 if axis == axis_at else 1 for axis in range(len(extent))])
    return level


def centred(rng, shape, scale, limit, pieces=(), held_as=jnp.bfloat16):
    drawn = jax.random.normal(rng, shape, jnp.float32) * scale
    if len(pieces) > 0:
        drawn = level_of(rng, shape, pieces, -0.22, 0.18) * drawn
    return jnp.clip(drawn, min=-limit, max=limit).astype(held_as)


def setup_inputs(seed: int = 0) -> dict:
    streams_of = jax.random.split(jax.random.key(seed), 10)
    queries = draw_queries(jax.random.fold_in(streams_of[9], 71), 0)
    keys = draw_keys(jax.random.fold_in(streams_of[9], 71), 0)
    values = centred(streams_of[2], (SEQUENCE_TOKENS, HEADS * HEAD_DIM), 4.0, 24.0, ((0, 8), (1, 4)))
    cum_gate = draw_cum_gate(jax.random.fold_in(streams_of[9], 71), 0)
    residual = centred(streams_of[4], (SEQUENCE_TOKENS, D), 0.25, 1.5, ((0, 32),))
    w_out = centred(streams_of[5], (HEADS * HEAD_DIM, D), (HEADS * HEAD_DIM) ** -0.5, 0.1875)
    gain = jnp.clip(1.0 + 0.18 * jax.random.normal(streams_of[6], (D,), jnp.float32), 0.1, 1.9)
    w_up = centred(streams_of[7], (D, FF), D ** -0.5, 0.125, ((0, 8), (1, 4)))
    w_down = centred(streams_of[8], (FF, D), FF ** -0.5, 0.0625, ((0, 4), (1, 8)))
    return dict(queries=queries, keys=keys, values=values, cum_gate=cum_gate, residual=residual, w_out=w_out, gain=gain, w_up=w_up, w_down=w_down)


def reference(queries, keys, values, cum_gate, residual, w_out, gain, w_up, w_down):
    width = HEADS * HEAD_DIM
    q_block = math.gcd(SEQUENCE_TOKENS, 512)
    key_heads = keys.astype(jnp.float32).reshape(SEQUENCE_TOKENS, HEADS, HEAD_DIM)
    value_heads = values.astype(jnp.float32).reshape(SEQUENCE_TOKENS, HEADS, HEAD_DIM)
    key_pos = jnp.arange(SEQUENCE_TOKENS, dtype=jnp.int32)
    gate_rows = cum_gate.T

    def attend(block_index):
        offset = (block_index * q_block).astype(jnp.int32)
        query_blk = lax.dynamic_slice_in_dim(queries, offset, q_block, 0).astype(jnp.float32)
        query_blk = query_blk.reshape(q_block, HEADS, HEAD_DIM)
        gate_blk = lax.dynamic_slice_in_dim(cum_gate, offset, q_block, 0)
        scores = jnp.einsum('qhd,khd->qhk', query_blk, key_heads) * HEAD_DIM ** (-0.5)
        scores = scores + gate_blk[:, :, None] - gate_rows[None, :, :]
        query_pos = offset + jnp.arange(q_block, dtype=jnp.int32)
        scores = jnp.where(key_pos[None, None, :] <= query_pos[:, None, None], scores, -1e+30)
        top = lax.optimization_barrier(jnp.max(scores, axis=-1, keepdims=True))
        weights = jnp.exp(scores - top)
        denom = lax.optimization_barrier(jnp.sum(weights, axis=-1))
        rounded = lax.optimization_barrier(weights.astype(jnp.bfloat16)).astype(jnp.float32)
        numer = jnp.einsum('qhk,khd->qhd', rounded, value_heads)
        return (numer / denom[:, :, None]).reshape(q_block, width).astype(jnp.bfloat16)
    blocks = lax.map(attend, jnp.arange(SEQUENCE_TOKENS // q_block, dtype=jnp.int32))
    attended = blocks.reshape(SEQUENCE_TOKENS, width)
    residual_sum = residual.astype(jnp.float32) + jnp.dot(attended, w_out, preferred_element_type=jnp.float32)
    mean_square = lax.optimization_barrier(jnp.mean(residual_sum * residual_sum, axis=-1, keepdims=True))
    normed = (residual_sum * lax.rsqrt(mean_square + 1e-06) * gain).astype(jnp.bfloat16)
    up_proj = jnp.dot(normed, w_up, preferred_element_type=jnp.float32)
    hidden = jnp.square(jax.nn.relu(up_proj)).astype(jnp.bfloat16)
    group = FF // N_TP
    summed = jnp.zeros((SEQUENCE_TOKENS, D), jnp.float32)
    for index in range(N_TP):
        part_out = jnp.dot(hidden[:, index * group:(index + 1) * group], w_down[index * group:(index + 1) * group], preferred_element_type=jnp.float32).astype(jnp.bfloat16)
        summed = summed + lax.optimization_barrier(part_out).astype(jnp.float32)
    return (residual_sum + summed).astype(jnp.bfloat16)
```

```python
import functools
import math

import jax
import jax.numpy as jnp
from jax import lax
from jax.experimental import pallas as pl
from jax.experimental.pallas import tpu as pltpu
from jax.sharding import PartitionSpec as P

LOG2E = math.log2(math.e)
NEG = -1e30


def body(
    n_sp, n_tp, heads,
    q_ref, kv_ref, gate_ref, res_ref, wout_hbm, gain_ref, wup_hbm, wdn_hbm,
    out_ref,
    kv_all, gate_all, m_s, l_s, acc_s, att, att_in, wout, rsum,
    wu, wd, norm_all, hid, psend, precv,
    kv_s1, kv_s2, kv_r, g_s1, g_s2, g_r, u_s1, u_s2, u_r, d_s1, d_s2, d_r,
    a_s, a_r, n_s, n_r, p_s, p_r, loc,
):
    ny = n_tp // 2
    nz = n_sp // ny
    tok, width = q_ref.shape
    hd = width // heads
    rows = tok // n_tp
    group = 2 * n_tp
    half = wu.shape[1]
    up_rows = wup_hbm.shape[0]
    features = res_ref.shape[1]
    cs = wdn_hbm.shape[1]
    me = lax.axis_index("sp")
    tp = lax.axis_index("tp")
    z, y = me // ny, me % ny
    par = z % 2
    slot = par * n_tp + tp

    def rcopy(src, dst, ss, rs, sp_to, tp_to=None):
        where = {"sp": sp_to} if tp_to is None else {"sp": sp_to, "tp": tp_to}
        return pltpu.make_async_remote_copy(
            src_ref=src, dst_ref=dst, send_sem=ss, recv_sem=rs,
            device_id=where, device_id_type=pl.DeviceIdType.MESH,
        )

    def member(o):
        other = (slot + o) % group
        return other, (z - par + other // n_tp) * ny + y, other % n_tp

    barrier = pltpu.get_barrier_semaphore()
    for dz in range(1, nz):
        pl.semaphore_signal(barrier, inc=1, device_id={"sp": ((z + dz) % nz) * ny + y},
                            device_id_type=pl.DeviceIdType.MESH)
    for dy in range(1, ny):
        pl.semaphore_signal(barrier, inc=1, device_id={"sp": z * ny + (y + dy) % ny},
                            device_id_type=pl.DeviceIdType.MESH)
    for o in range(1, group):
        _, sp_to, tp_to = member(o)
        pl.semaphore_signal(barrier, inc=1, device_id={"sp": sp_to, "tp": tp_to},
                            device_id_type=pl.DeviceIdType.MESH)
    pl.semaphore_wait(barrier, nz - 1 + ny - 1 + group - 1)

    def kv_first(dz):
        to = (z + dz) * ny + y
        return (rcopy(kv_ref, kv_all.at[me], kv_s1.at[dz], kv_r.at[me], to),
                rcopy(gate_ref, gate_all.at[me], g_s1.at[dz], g_r.at[me], to))

    def kv_own(dy):
        to = z * ny + (y + dy) % ny
        return (rcopy(kv_ref, kv_all.at[me], kv_s2.at[z * ny + dy], kv_r.at[me], to),
                rcopy(gate_ref, gate_all.at[me], g_s2.at[z * ny + dy], g_r.at[me], to))

    def kv_forward(zs, dy):
        s = zs * ny + y
        to = z * ny + (y + dy) % ny
        return (rcopy(kv_all.at[s], kv_all.at[s], kv_s2.at[zs * ny + dy], kv_r.at[s], to),
                rcopy(gate_all.at[s], gate_all.at[s], g_s2.at[zs * ny + dy], g_r.at[s], to))

    def wu_at(s):
        return wu.at[pl.ds(pl.multiple_of(s * up_rows, up_rows), up_rows), :]

    def up_half(p):
        return wup_hbm.at[:, pl.ds(pl.multiple_of(p * half, half), half)]

    def dn_half(p):
        return wdn_hbm.at[pl.ds(pl.multiple_of(p * half, half), half), :]

    def up_first(dz):
        zt = (z + dz) % nz
        return rcopy(up_half(zt % 2), wu_at(me), u_s1.at[dz], u_r.at[me], zt * ny + y)

    def dn_first(dz):
        zt = (z + dz) % nz
        return rcopy(dn_half(zt % 2), wd.at[me], d_s1.at[dz], d_r.at[me], zt * ny + y)

    def up_own(dy):
        return rcopy(up_half(par), wu_at(me), u_s2.at[z * ny + dy], u_r.at[me], z * ny + (y + dy) % ny)

    def dn_own(dy):
        return rcopy(dn_half(par), wd.at[me], d_s2.at[z * ny + dy], d_r.at[me], z * ny + (y + dy) % ny)

    def up_forward(zs, dy):
        s = zs * ny + y
        return rcopy(wu_at(s), wu_at(s), u_s2.at[zs * ny + dy], u_r.at[s], z * ny + (y + dy) % ny)

    def dn_forward(zs, dy):
        s = zs * ny + y
        return rcopy(wd.at[s], wd.at[s], d_s2.at[zs * ny + dy], d_r.at[s], z * ny + (y + dy) % ny)

    for dz in range(1, nz):
        @pl.when(z + dz < nz)
        def _(dz=dz):
            for c in kv_first(dz):
                c.start()
    for dy in range(1, ny):
        @pl.when((y + dy) % ny > y)
        def _(dy=dy):
            for c in kv_own(dy):
                c.start()
    local_wout = pltpu.make_async_copy(wout_hbm, wout, loc.at[0])
    local_up = pltpu.make_async_copy(up_half(par), wu_at(me), loc.at[1])
    local_dn = pltpu.make_async_copy(dn_half(par), wd.at[me], loc.at[2])
    local_wout.start()
    local_up.start()
    local_dn.start()
    for dz in range(1, nz):
        up_first(dz).start()
    for dy in range(1, ny):
        up_own(dy).start()
    for dz in range(1, nz):
        dn_first(dz).start()
    for dy in range(1, ny):
        dn_own(dy).start()

    scale = hd ** (-0.5) * LOG2E

    def absorb(kv, gates, diagonal):
        for h in range(heads):
            cols = pl.ds(h * hd, hd)
            rel = (gates[h:h + 1, :] - gate_ref[h:h + 1, 0:1]) * LOG2E
            s = lax.dot_general(q_ref[:, cols], kv[:, cols], (((1,), (1,)), ((), ())),
                                preferred_element_type=jnp.float32)
            s = s * scale - rel
            if diagonal:
                qp = lax.broadcasted_iota(jnp.int32, s.shape, 0)
                kp = lax.broadcasted_iota(jnp.int32, s.shape, 1)
                s = jnp.where(kp <= qp, s, NEG)
            top = jnp.max(s, axis=1, keepdims=True)
            if not diagonal:
                old = m_s[:, h:h + 1]
                top = jnp.maximum(old, top)
                fade = jnp.exp2(old - top)
            w = jnp.exp2(s - top)
            total = jnp.sum(w, axis=1, keepdims=True)
            add = jnp.dot(w.astype(jnp.bfloat16), kv[:, pl.ds(width + h * hd, hd)],
                          preferred_element_type=jnp.float32)
            if not diagonal:
                total = l_s[:, h:h + 1] * fade + total
                add = acc_s[:, cols] * fade + add
            m_s[:, h:h + 1] = top
            l_s[:, h:h + 1] = total
            acc_s[:, cols] = add

    absorb(kv_ref, gate_ref, True)

    def level(i, carry):
        zs = z - i

        @pl.when(zs >= 0)
        def _():
            @pl.when(i > 0)
            def _():
                own = zs * ny + y
                rcopy(kv_ref, kv_all.at[own], kv_s1.at[0], kv_r.at[own], me).wait_recv()
                rcopy(gate_ref, gate_all.at[own], g_s1.at[0], g_r.at[own], me).wait_recv()
                for dy in range(1, ny):
                    for c in kv_forward(zs, dy):
                        c.start()

            def column(dy, carry):
                s = zs * ny + (y + dy) % ny

                @pl.when(s < me)
                def _():
                    @pl.when(dy > 0)
                    def _():
                        rcopy(kv_ref, kv_all.at[s], kv_s1.at[0], kv_r.at[s], me).wait_recv()
                        rcopy(gate_ref, gate_all.at[s], g_s1.at[0], g_r.at[s], me).wait_recv()
                    absorb(kv_all.at[s], gate_all.at[s], False)
                return carry

            lax.fori_loop(0, ny, column, 0)
        return carry

    lax.fori_loop(0, nz, level, 0)

    for h in range(heads):
        cols = pl.ds(h * hd, hd)
        done = (acc_s[:, cols] / l_s[:, h:h + 1]).astype(jnp.bfloat16)
        for j in range(n_tp):
            att[j, :, cols] = done[j * rows:(j + 1) * rows, :]

    def heads_to(o):
        to = (tp + o) % n_tp
        return rcopy(att.at[to], att_in.at[tp], a_s.at[o], a_r.at[tp], me, to)

    for o in range(1, n_tp):
        heads_to(o).start()
    att_in[pl.ds(tp, 1)] = att[pl.ds(tp, 1)]
    local_wout.wait()
    for o in range(1, n_tp):
        src = (tp + o) % n_tp
        rcopy(att.at[0], att_in.at[src], a_s.at[0], a_r.at[src], me, tp).wait_recv()
    total = res_ref[...].astype(jnp.float32)
    for j in range(n_tp):
        total += jnp.dot(att_in[j], wout[j * width:(j + 1) * width, :], preferred_element_type=jnp.float32)
    rsum[...] = total
    mean_square = jnp.mean(total * total, axis=-1, keepdims=True)
    normed = (total * lax.rsqrt(mean_square + 1e-06) * gain_ref[...]).astype(jnp.bfloat16)

    def block(ref, b):
        return ref.at[pl.ds(pl.multiple_of(b * rows, rows), rows), :]

    block(norm_all, slot)[...] = normed

    def normed_to(o):
        _, sp_to, tp_to = member(o)
        return rcopy(block(norm_all, slot), block(norm_all, slot), n_s.at[o], n_r.at[slot], sp_to, tp_to)

    for o in range(1, group):
        normed_to(o).start()

    for dz in range(1, nz):
        zs = (z - dz + nz) % nz
        s = zs * ny + y
        rcopy(up_half(0), wu_at(s), u_s1.at[0], u_r.at[s], me).wait_recv()
        for dy in range(1, ny):
            up_forward(zs, dy).start()
    for dz in range(1, nz):
        zs = (z - dz + nz) % nz
        s = zs * ny + y
        rcopy(dn_half(0), wd.at[s], d_s1.at[0], d_r.at[s], me).wait_recv()
        for dy in range(1, ny):
            dn_forward(zs, dy).start()
    local_up.wait()
    local_dn.wait()
    for dy in range(1, ny):
        for zs in range(nz):
            s = zs * ny + (y + dy) % ny
            rcopy(up_half(0), wu_at(s), u_s1.at[0], u_r.at[s], me).wait_recv()
    for o in range(1, group):
        src = (slot + o) % group
        rcopy(block(norm_all, src), block(norm_all, src), n_s.at[0], n_r.at[src], me).wait_recv()

    tile = min(256, half)

    def up_tile(i, carry):
        cols = pl.ds(pl.multiple_of(i * tile, tile), tile)
        u = jnp.maximum(jnp.dot(norm_all[...], wu[:, cols], preferred_element_type=jnp.float32), 0.0)
        hid[:, cols] = (u * u).astype(jnp.bfloat16)
        return carry

    lax.fori_loop(0, half // tile, up_tile, 0)
    for dy in range(1, ny):
        for zs in range(nz):
            s = zs * ny + (y + dy) % ny
            rcopy(dn_half(0), wd.at[s], d_s1.at[0], d_r.at[s], me).wait_recv()

    per = max(1, 128 // cs)

    def dn_tile(i, carry):
        if per == 1:
            w = wd[i]
        else:
            w = jnp.concatenate([wd[i * per + k] for k in range(per)], axis=1)
        cols = pl.ds(pl.multiple_of(i * per * cs, per * cs), per * cs)
        psend[:, cols] = jnp.dot(hid[...], w, preferred_element_type=jnp.float32).astype(jnp.bfloat16)
        return carry

    lax.fori_loop(0, features // (per * cs), dn_tile, 0)

    def partial_to(o):
        other, sp_to, tp_to = member(o)
        return rcopy(block(psend, other), block(precv, slot), p_s.at[o], p_r.at[slot], sp_to, tp_to)

    for o in range(1, group):
        partial_to(o).start()
    total = rsum[...] + block(psend, slot)[...].astype(jnp.float32)
    for o in range(1, group):
        src = (slot + o) % group
        rcopy(block(psend, src), block(precv, src), p_s.at[0], p_r.at[src], me).wait_recv()
        total += block(precv, src)[...].astype(jnp.float32)
    out_ref[...] = total.astype(jnp.bfloat16)

    for dz in range(1, nz):
        @pl.when(z + dz < nz)
        def _(dz=dz):
            for c in kv_first(dz):
                c.wait_send()
        up_first(dz).wait_send()
        dn_first(dz).wait_send()
    for dy in range(1, ny):
        @pl.when((y + dy) % ny > y)
        def _(dy=dy):
            for c in kv_own(dy):
                c.wait_send()
        up_own(dy).wait_send()
        dn_own(dy).wait_send()
        for dz in range(1, nz):
            zs = (z - dz + nz) % nz

            @pl.when(z - dz >= 0)
            def _(zs=zs, dy=dy):
                for c in kv_forward(zs, dy):
                    c.wait_send()
            up_forward(zs, dy).wait_send()
            dn_forward(zs, dy).wait_send()
    for o in range(1, n_tp):
        heads_to(o).wait_send()
    for o in range(1, group):
        normed_to(o).wait_send()
        partial_to(o).wait_send()


def per_device(n_sp, n_tp, queries, keys, values, cum_gate, residual, w_out, gain, w_up, w_down):
    tok, width = queries.shape
    heads = cum_gate.shape[1]
    rows, features = residual.shape
    ny = n_tp // 2
    nz = n_sp // ny
    group = 2 * n_tp
    half = w_up.shape[1] // 2
    bf, f32 = jnp.bfloat16, jnp.float32
    gates = jnp.pad(cum_gate.T, ((0, 8 - heads), (0, 0)))
    kv = jnp.concatenate([keys, values], axis=1)
    vmem = pl.BlockSpec(memory_space=pltpu.VMEM)
    hbm = pl.BlockSpec(memory_space=pl.ANY)
    dma = lambda n: pltpu.SemaphoreType.DMA((n,))
    return pl.pallas_call(
        functools.partial(body, n_sp, n_tp, heads),
        out_shape=jax.ShapeDtypeStruct((rows, features), bf),
        in_specs=[vmem, vmem, vmem, vmem, hbm, vmem, hbm, hbm],
        out_specs=vmem,
        scratch_shapes=[
            pltpu.VMEM((n_sp, tok, 2 * width), bf),
            pltpu.VMEM((n_sp,) + gates.shape, f32),
            pltpu.VMEM((tok, 128), f32),
            pltpu.VMEM((tok, 128), f32),
            pltpu.VMEM((tok, width), f32),
            pltpu.VMEM((n_tp, rows, width), bf),
            pltpu.VMEM((n_tp, rows, width), bf),
            pltpu.VMEM(w_out.shape, bf),
            pltpu.VMEM((rows, features), f32),
            pltpu.VMEM((n_sp * w_up.shape[0], half), bf),
            pltpu.VMEM((n_sp, half, w_down.shape[1]), bf),
            pltpu.VMEM((group * rows, features), bf),
            pltpu.VMEM((group * rows, half), bf),
            pltpu.VMEM((group * rows, features), bf),
            pltpu.VMEM((group * rows, features), bf),
        ]
        + [dma(nz), dma(n_sp), dma(n_sp)] * 4
        + [dma(n_tp), dma(n_tp), dma(group), dma(group), dma(group), dma(group), dma(3)],
        compiler_params=pltpu.CompilerParams(
            collective_id=0, has_side_effects=True, vmem_limit_bytes=63 * 1024 * 1024
        ),
    )(queries, kv, gates, residual, w_out, gain.reshape(1, -1), w_up, w_down)


def solution(mesh):
    n_sp, n_tp = mesh.shape["sp"], mesh.shape["tp"]
    return jax.shard_map(
        functools.partial(per_device, n_sp, n_tp),
        mesh=mesh,
        in_specs=(
            P("sp", "tp"),
            P("sp", "tp"),
            P("sp", "tp"),
            P("sp", "tp"),
            P(("sp", "tp"), None),
            P(),
            P(),
            P("sp", "tp"),
            P("tp", "sp"),
        ),
        out_specs=P(("sp", "tp"), None),
        check_vma=False,
    )
```

```python
import functools
import math

import jax
import jax.numpy as jnp
from jax import lax
from jax.experimental import pallas as pl
from jax.experimental.pallas import tpu as pltpu
from jax.sharding import PartitionSpec as P

LOG2E = math.log2(math.e)
NEG = -1e30


def body(
    n_sp, n_tp, heads,
    q_ref, kv_ref, gate_ref, res_ref, wout_hbm, gain_ref, wup_hbm, wdn_hbm,
    out_ref,
    kv_all, gate_all, m_s, l_s, acc_s, att, att_in, wout, rsum,
    wu, wd, norm_all, hid, psend, precv,
    kv_s1, kv_s2, kv_r, g_s1, g_s2, g_r, u_s1, u_s2, u_r, d_s1, d_s2, d_r,
    a_s, a_r, n_s, n_r, p_s, p_r, loc,
):
    ny = n_tp // 2
    nz = n_sp // ny
    tok, width = q_ref.shape
    hd = width // heads
    rows = tok // n_tp
    group = 2 * n_tp
    half = wu.shape[1]
    up_rows = wup_hbm.shape[0]
    features = res_ref.shape[1]
    cs = wdn_hbm.shape[1]
    me = lax.axis_index("sp")
    tp = lax.axis_index("tp")
    z, y = me // ny, me % ny
    par = z % 2
    slot = par * n_tp + tp

    def rcopy(src, dst, ss, rs, sp_to, tp_to=None):
        where = {"sp": sp_to} if tp_to is None else {"sp": sp_to, "tp": tp_to}
        return pltpu.make_async_remote_copy(
            src_ref=src, dst_ref=dst, send_sem=ss, recv_sem=rs,
            device_id=where, device_id_type=pl.DeviceIdType.MESH,
        )

    def member(o):
        other = (slot + o) % group
        return other, (z - par + other // n_tp) * ny + y, other % n_tp

    barrier = pltpu.get_barrier_semaphore()
    for dz in range(1, nz):
        pl.semaphore_signal(barrier, inc=1, device_id={"sp": ((z + dz) % nz) * ny + y},
                            device_id_type=pl.DeviceIdType.MESH)
    for dy in range(1, ny):
        pl.semaphore_signal(barrier, inc=1, device_id={"sp": z * ny + (y + dy) % ny},
                            device_id_type=pl.DeviceIdType.MESH)
    for o in range(1, group):
        _, sp_to, tp_to = member(o)
        pl.semaphore_signal(barrier, inc=1, device_id={"sp": sp_to, "tp": tp_to},
                            device_id_type=pl.DeviceIdType.MESH)
    pl.semaphore_wait(barrier, nz - 1 + ny - 1 + group - 1)

    def kv_first(dz):
        to = (z + dz) * ny + y
        return (rcopy(kv_ref, kv_all.at[me], kv_s1.at[dz], kv_r.at[me], to),
                rcopy(gate_ref, gate_all.at[me], g_s1.at[dz], g_r.at[me], to))

    def kv_own(dy):
        to = z * ny + (y + dy) % ny
        return (rcopy(kv_ref, kv_all.at[me], kv_s2.at[z * ny + dy], kv_r.at[me], to),
                rcopy(gate_ref, gate_all.at[me], g_s2.at[z * ny + dy], g_r.at[me], to))

    def kv_forward(zs, dy):
        s = zs * ny + y
        to = z * ny + (y + dy) % ny
        return (rcopy(kv_all.at[s], kv_all.at[s], kv_s2.at[zs * ny + dy], kv_r.at[s], to),
                rcopy(gate_all.at[s], gate_all.at[s], g_s2.at[zs * ny + dy], g_r.at[s], to))

    def wu_at(s):
        return wu.at[pl.ds(pl.multiple_of(s * up_rows, up_rows), up_rows), :]

    def up_half(p):
        return wup_hbm.at[:, pl.ds(pl.multiple_of(p * half, half), half)]

    def dn_half(p):
        return wdn_hbm.at[pl.ds(pl.multiple_of(p * half, half), half), :]

    def up_first(dz):
        zt = (z + dz) % nz
        return rcopy(up_half(zt % 2), wu_at(me), u_s1.at[dz], u_r.at[me], zt * ny + y)

    def dn_first(dz):
        zt = (z + dz) % nz
        return rcopy(dn_half(zt % 2), wd.at[me], d_s1.at[dz], d_r.at[me], zt * ny + y)

    def up_own(dy):
        return rcopy(up_half(par), wu_at(me), u_s2.at[z * ny + dy], u_r.at[me], z * ny + (y + dy) % ny)

    def dn_own(dy):
        return rcopy(dn_half(par), wd.at[me], d_s2.at[z * ny + dy], d_r.at[me], z * ny + (y + dy) % ny)

    def up_forward(zs, dy):
        s = zs * ny + y
        return rcopy(wu_at(s), wu_at(s), u_s2.at[zs * ny + dy], u_r.at[s], z * ny + (y + dy) % ny)

    def dn_forward(zs, dy):
        s = zs * ny + y
        return rcopy(wd.at[s], wd.at[s], d_s2.at[zs * ny + dy], d_r.at[s], z * ny + (y + dy) % ny)

    for dz in range(1, nz):
        @pl.when(z + dz < nz)
        def _(dz=dz):
            for c in kv_first(dz):
                c.start()
    for dy in range(1, ny):
        @pl.when((y + dy) % ny > y)
        def _(dy=dy):
            for c in kv_own(dy):
                c.start()
    local_wout = pltpu.make_async_copy(wout_hbm, wout, loc.at[0])
    local_up = pltpu.make_async_copy(up_half(par), wu_at(me), loc.at[1])
    local_dn = pltpu.make_async_copy(dn_half(par), wd.at[me], loc.at[2])
    local_wout.start()
    local_up.start()
    local_dn.start()
    for dz in range(1, nz):
        up_first(dz).start()
    for dy in range(1, ny):
        up_own(dy).start()

    scale = hd ** (-0.5) * LOG2E

    def absorb(kv, gates, diagonal):
        for h in range(heads):
            cols = pl.ds(h * hd, hd)
            rel = (gates[h:h + 1, :] - gate_ref[h:h + 1, 0:1]) * LOG2E
            s = lax.dot_general(q_ref[:, cols], kv[:, cols], (((1,), (1,)), ((), ())),
                                preferred_element_type=jnp.float32)
            s = s * scale - rel
            if diagonal:
                qp = lax.broadcasted_iota(jnp.int32, s.shape, 0)
                kp = lax.broadcasted_iota(jnp.int32, s.shape, 1)
                s = jnp.where(kp <= qp, s, NEG)
            top = jnp.max(s, axis=1, keepdims=True)
            if not diagonal:
                old = m_s[:, h:h + 1]
                top = jnp.maximum(old, top)
                fade = jnp.exp2(old - top)
            w = jnp.exp2(s - top)
            total = jnp.sum(w, axis=1, keepdims=True)
            add = jnp.dot(w.astype(jnp.bfloat16), kv[:, pl.ds(width + h * hd, hd)],
                          preferred_element_type=jnp.float32)
            if not diagonal:
                total = l_s[:, h:h + 1] * fade + total
                add = acc_s[:, cols] * fade + add
            m_s[:, h:h + 1] = top
            l_s[:, h:h + 1] = total
            acc_s[:, cols] = add

    absorb(kv_ref, gate_ref, True)

    def level(i, carry):
        zs = z - i

        @pl.when(zs >= 0)
        def _():
            @pl.when(i > 0)
            def _():
                own = zs * ny + y
                rcopy(kv_ref, kv_all.at[own], kv_s1.at[0], kv_r.at[own], me).wait_recv()
                rcopy(gate_ref, gate_all.at[own], g_s1.at[0], g_r.at[own], me).wait_recv()
                for dy in range(1, ny):
                    for c in kv_forward(zs, dy):
                        c.start()

            def column(dy, carry):
                s = zs * ny + (y + dy) % ny

                @pl.when(s < me)
                def _():
                    @pl.when(dy > 0)
                    def _():
                        rcopy(kv_ref, kv_all.at[s], kv_s1.at[0], kv_r.at[s], me).wait_recv()
                        rcopy(gate_ref, gate_all.at[s], g_s1.at[0], g_r.at[s], me).wait_recv()
                    absorb(kv_all.at[s], gate_all.at[s], False)
                return carry

            lax.fori_loop(0, ny, column, 0)
        return carry

    lax.fori_loop(0, nz, level, 0)

    for h in range(heads):
        cols = pl.ds(h * hd, hd)
        done = (acc_s[:, cols] / l_s[:, h:h + 1]).astype(jnp.bfloat16)
        for j in range(n_tp):
            att[j, :, cols] = done[j * rows:(j + 1) * rows, :]

    def heads_to(o):
        to = (tp + o) % n_tp
        return rcopy(att.at[to], att_in.at[tp], a_s.at[o], a_r.at[tp], me, to)

    for o in range(1, n_tp):
        heads_to(o).start()
    att_in[pl.ds(tp, 1)] = att[pl.ds(tp, 1)]
    local_wout.wait()
    for o in range(1, n_tp):
        src = (tp + o) % n_tp
        rcopy(att.at[0], att_in.at[src], a_s.at[0], a_r.at[src], me, tp).wait_recv()
    total = res_ref[...].astype(jnp.float32)
    for j in range(n_tp):
        total += jnp.dot(att_in[j], wout[j * width:(j + 1) * width, :], preferred_element_type=jnp.float32)
    rsum[...] = total
    mean_square = jnp.mean(total * total, axis=-1, keepdims=True)
    normed = (total * lax.rsqrt(mean_square + 1e-06) * gain_ref[...]).astype(jnp.bfloat16)

    def block(ref, b):
        return ref.at[pl.ds(pl.multiple_of(b * rows, rows), rows), :]

    block(norm_all, slot)[...] = normed

    def normed_row(src, sem, other):
        zo, to = other // n_tp, other % n_tp
        return rcopy(block(norm_all, src), block(norm_all, src), n_s.at[sem], n_r.at[src],
                     (z - par + zo) * ny + y, to)

    chips = group // 2
    core = tp % 2
    mate = slot + 1 - 2 * core

    def normed_chip(k):
        return normed_row(slot, k, (slot + 2 * k) % group)

    def normed_mate(k):
        return normed_row((slot + 2 * k) % group, chips + k, mate)

    for k in range(1, chips):
        normed_chip(k).start()
    normed_mate(0).start()
    for dz in range(1, nz):
        dn_first(dz).start()
    for dy in range(1, ny):
        dn_own(dy).start()

    for dz in range(1, nz):
        zs = (z - dz + nz) % nz
        s = zs * ny + y
        rcopy(up_half(0), wu_at(s), u_s1.at[0], u_r.at[s], me).wait_recv()
        for dy in range(1, ny):
            up_forward(zs, dy).start()
    for k in range(1, chips):
        src = (slot + 2 * k) % group
        rcopy(block(norm_all, src), block(norm_all, src), n_s.at[0], n_r.at[src], me).wait_recv()
        normed_mate(k).start()

    def down_on(dz):
        zs = (z - dz + nz) % nz
        s = zs * ny + y
        rcopy(dn_half(0), wd.at[s], d_s1.at[0], d_r.at[s], me).wait_recv()
        for dy in range(1, ny):
            dn_forward(zs, dy).start()

    local_up.wait()
    for dy in range(1, ny):
        for zs in range(nz):
            s = zs * ny + (y + dy) % ny
            rcopy(up_half(0), wu_at(s), u_s1.at[0], u_r.at[s], me).wait_recv()
    for k in range(chips):
        src = (mate + 2 * k) % group
        rcopy(block(norm_all, src), block(norm_all, src), n_s.at[0], n_r.at[src], me).wait_recv()

    tile = min(256, half)

    def up_tile(i, carry):
        cols = pl.ds(pl.multiple_of(i * tile, tile), tile)
        u = jnp.maximum(jnp.dot(norm_all[...], wu[:, cols], preferred_element_type=jnp.float32), 0.0)
        hid[:, cols] = (u * u).astype(jnp.bfloat16)
        return carry

    lax.fori_loop(0, half // tile, up_tile, 0)

    per = max(1, 128 // cs)
    span = ny * cs

    def part(ref, b, zs):
        return ref.at[pl.ds(pl.multiple_of(b * rows, rows), rows),
                      pl.ds(pl.multiple_of(zs * span, span), span)]

    def partial_to(o, zs):
        other, sp_to, tp_to = member(o)
        return rcopy(part(psend, other, zs), part(precv, slot, zs), p_s.at[o * nz + zs],
                     p_r.at[slot * nz + zs], sp_to, tp_to)

    def down_level(dz):
        zs = (z - dz + nz) % nz
        for k in range(ny // per):
            ws = [wd[zs * ny + k * per + i] for i in range(per)]
            w = ws[0] if per == 1 else jnp.concatenate(ws, axis=1)
            cols = pl.ds(pl.multiple_of((zs * ny + k * per) * cs, per * cs), per * cs)
            psend[:, cols] = jnp.dot(hid[...], w, preferred_element_type=jnp.float32).astype(jnp.bfloat16)
        for o in range(1, group):
            partial_to(o, zs).start()

    local_dn.wait()
    for dz in range(nz):
        if dz + 1 < nz:
            down_on(dz + 1)
        zs = (z - dz + nz) % nz
        for dy in range(1, ny):
            s = zs * ny + (y + dy) % ny
            rcopy(dn_half(0), wd.at[s], d_s1.at[0], d_r.at[s], me).wait_recv()
        down_level(dz)

    total = rsum[...] + block(psend, slot)[...].astype(jnp.float32)
    for o in range(1, group):
        src = (slot + o) % group
        for zs in range(nz):
            rcopy(part(psend, src, zs), part(precv, src, zs), p_s.at[0], p_r.at[src * nz + zs], me).wait_recv()
        total += block(precv, src)[...].astype(jnp.float32)
    out_ref[...] = total.astype(jnp.bfloat16)

    for dz in range(1, nz):
        @pl.when(z + dz < nz)
        def _(dz=dz):
            for c in kv_first(dz):
                c.wait_send()
        up_first(dz).wait_send()
        dn_first(dz).wait_send()
    for dy in range(1, ny):
        @pl.when((y + dy) % ny > y)
        def _(dy=dy):
            for c in kv_own(dy):
                c.wait_send()
        up_own(dy).wait_send()
        dn_own(dy).wait_send()
        for dz in range(1, nz):
            zs = (z - dz + nz) % nz

            @pl.when(z - dz >= 0)
            def _(zs=zs, dy=dy):
                for c in kv_forward(zs, dy):
                    c.wait_send()
            up_forward(zs, dy).wait_send()
            dn_forward(zs, dy).wait_send()
    for o in range(1, n_tp):
        heads_to(o).wait_send()
    for k in range(1, chips):
        normed_chip(k).wait_send()
    for k in range(chips):
        normed_mate(k).wait_send()
    for o in range(1, group):
        for zs in range(nz):
            partial_to(o, zs).wait_send()


def per_device(n_sp, n_tp, queries, keys, values, cum_gate, residual, w_out, gain, w_up, w_down):
    tok, width = queries.shape
    heads = cum_gate.shape[1]
    rows, features = residual.shape
    ny = n_tp // 2
    nz = n_sp // ny
    group = 2 * n_tp
    half = w_up.shape[1] // 2
    bf, f32 = jnp.bfloat16, jnp.float32
    gates = jnp.pad(cum_gate.T, ((0, 8 - heads), (0, 0)))
    kv = jnp.concatenate([keys, values], axis=1)
    vmem = pl.BlockSpec(memory_space=pltpu.VMEM)
    hbm = pl.BlockSpec(memory_space=pl.ANY)
    dma = lambda n: pltpu.SemaphoreType.DMA((n,))
    return pl.pallas_call(
        functools.partial(body, n_sp, n_tp, heads),
        out_shape=jax.ShapeDtypeStruct((rows, features), bf),
        in_specs=[vmem, vmem, vmem, vmem, hbm, vmem, hbm, hbm],
        out_specs=vmem,
        scratch_shapes=[
            pltpu.VMEM((n_sp, tok, 2 * width), bf),
            pltpu.VMEM((n_sp,) + gates.shape, f32),
            pltpu.VMEM((tok, 128), f32),
            pltpu.VMEM((tok, 128), f32),
            pltpu.VMEM((tok, width), f32),
            pltpu.VMEM((n_tp, rows, width), bf),
            pltpu.VMEM((n_tp, rows, width), bf),
            pltpu.VMEM(w_out.shape, bf),
            pltpu.VMEM((rows, features), f32),
            pltpu.VMEM((n_sp * w_up.shape[0], half), bf),
            pltpu.VMEM((n_sp, half, w_down.shape[1]), bf),
            pltpu.VMEM((group * rows, features), bf),
            pltpu.VMEM((group * rows, half), bf),
            pltpu.VMEM((group * rows, features), bf),
            pltpu.VMEM((group * rows, features), bf),
        ]
        + [dma(nz), dma(n_sp), dma(n_sp)] * 4
        + [dma(n_tp), dma(n_tp), dma(group), dma(group), dma(group * nz), dma(group * nz), dma(3)],
        compiler_params=pltpu.CompilerParams(
            collective_id=0, has_side_effects=True, vmem_limit_bytes=63 * 1024 * 1024
        ),
    )(queries, kv, gates, residual, w_out, gain.reshape(1, -1), w_up, w_down)


def solution(mesh):
    n_sp, n_tp = mesh.shape["sp"], mesh.shape["tp"]
    return jax.shard_map(
        functools.partial(per_device, n_sp, n_tp),
        mesh=mesh,
        in_specs=(
            P("sp", "tp"),
            P("sp", "tp"),
            P("sp", "tp"),
            P("sp", "tp"),
            P(("sp", "tp"), None),
            P(),
            P(),
            P("sp", "tp"),
            P("tp", "sp"),
        ),
        out_specs=P(("sp", "tp"), None),
        check_vma=False,
    )
```

```python
import functools
import math

import jax
import jax.numpy as jnp
from jax import lax
from jax.experimental import pallas as pl
from jax.experimental.pallas import tpu as pltpu
from jax.sharding import PartitionSpec as P

LOG2E = math.log2(math.e)
NEG = -1e30


def body(
    n_sp, n_tp, heads,
    q_ref, kv_ref, gate_ref, res_ref, wout_hbm, gain_ref, wup_hbm, wdn_hbm,
    out_ref,
    kv_all, gate_all, m_s, l_s, acc_s, att, att_in, wout, rsum,
    wu, wd, norm_all, hid, psend, pmate, pcomb, precv,
    kv_s1, kv_s2, kv_r, g_s1, g_s2, g_r, u_s1, u_s2, u_r, d_s1, d_s2, d_r,
    a_s, a_r, n_s, n_r, p_s, p_r, q_s, q_r, loc,
):
    ny = n_tp // 2
    nz = n_sp // ny
    tok, width = q_ref.shape
    hd = width // heads
    rows = tok // n_tp
    group = 2 * n_tp
    half = wu.shape[1]
    up_rows = wup_hbm.shape[0]
    features = res_ref.shape[1]
    cs = wdn_hbm.shape[1]
    me = lax.axis_index("sp")
    tp = lax.axis_index("tp")
    z, y = me // ny, me % ny
    par = z % 2
    slot = par * n_tp + tp

    def rcopy(src, dst, ss, rs, sp_to, tp_to=None):
        where = {"sp": sp_to} if tp_to is None else {"sp": sp_to, "tp": tp_to}
        return pltpu.make_async_remote_copy(
            src_ref=src, dst_ref=dst, send_sem=ss, recv_sem=rs,
            device_id=where, device_id_type=pl.DeviceIdType.MESH,
        )

    def member(o):
        other = (slot + o) % group
        return other, (z - par + other // n_tp) * ny + y, other % n_tp

    barrier = pltpu.get_barrier_semaphore()
    for dz in range(1, nz):
        pl.semaphore_signal(barrier, inc=1, device_id={"sp": ((z + dz) % nz) * ny + y},
                            device_id_type=pl.DeviceIdType.MESH)
    for dy in range(1, ny):
        pl.semaphore_signal(barrier, inc=1, device_id={"sp": z * ny + (y + dy) % ny},
                            device_id_type=pl.DeviceIdType.MESH)
    for o in range(1, group):
        _, sp_to, tp_to = member(o)
        pl.semaphore_signal(barrier, inc=1, device_id={"sp": sp_to, "tp": tp_to},
                            device_id_type=pl.DeviceIdType.MESH)
    pl.semaphore_wait(barrier, nz - 1 + ny - 1 + group - 1)

    def kv_up(zs):
        s = zs * ny + y
        to = me + ny
        return (rcopy(kv_all.at[s], kv_all.at[s], kv_s1.at[zs], kv_r.at[s], to),
                rcopy(gate_all.at[s], gate_all.at[s], g_s1.at[zs], g_r.at[s], to))

    def kv_first():
        to = me + ny
        return (rcopy(kv_ref, kv_all.at[me], kv_s1.at[z], kv_r.at[me], to),
                rcopy(gate_ref, gate_all.at[me], g_s1.at[z], g_r.at[me], to))

    def kv_own(dy):
        to = z * ny + (y + dy) % ny
        return (rcopy(kv_ref, kv_all.at[me], kv_s2.at[z * ny + dy], kv_r.at[me], to),
                rcopy(gate_ref, gate_all.at[me], g_s2.at[z * ny + dy], g_r.at[me], to))

    def kv_forward(zs, dy):
        s = zs * ny + y
        to = z * ny + (y + dy) % ny
        return (rcopy(kv_all.at[s], kv_all.at[s], kv_s2.at[zs * ny + dy], kv_r.at[s], to),
                rcopy(gate_all.at[s], gate_all.at[s], g_s2.at[zs * ny + dy], g_r.at[s], to))

    def wu_at(s):
        return wu.at[pl.ds(pl.multiple_of(s * up_rows, up_rows), up_rows), :]

    def up_half(p):
        return wup_hbm.at[:, pl.ds(pl.multiple_of(p * half, half), half)]

    def dn_half(p):
        return wdn_hbm.at[pl.ds(pl.multiple_of(p * half, half), half), :]

    def up_first(dz):
        zt = (z + dz) % nz
        return rcopy(up_half(zt % 2), wu_at(me), u_s1.at[dz], u_r.at[me], zt * ny + y)

    def dn_first(dz):
        zt = (z + dz) % nz
        return rcopy(dn_half(zt % 2), wd.at[me], d_s1.at[dz], d_r.at[me], zt * ny + y)

    def up_own(dy):
        return rcopy(up_half(par), wu_at(me), u_s2.at[z * ny + dy], u_r.at[me], z * ny + (y + dy) % ny)

    def dn_own(dy):
        return rcopy(dn_half(par), wd.at[me], d_s2.at[z * ny + dy], d_r.at[me], z * ny + (y + dy) % ny)

    def up_forward(zs, dy):
        s = zs * ny + y
        return rcopy(wu_at(s), wu_at(s), u_s2.at[zs * ny + dy], u_r.at[s], z * ny + (y + dy) % ny)

    def dn_forward(zs, dy):
        s = zs * ny + y
        return rcopy(wd.at[s], wd.at[s], d_s2.at[zs * ny + dy], d_r.at[s], z * ny + (y + dy) % ny)

    @pl.when(z + 1 < nz)
    def _():
        for c in kv_first():
            c.start()
    for dy in range(1, ny):
        @pl.when((y + dy) % ny > y)
        def _(dy=dy):
            for c in kv_own(dy):
                c.start()
    local_wout = pltpu.make_async_copy(wout_hbm, wout, loc.at[0])
    local_up = pltpu.make_async_copy(up_half(par), wu_at(me), loc.at[1])
    local_dn = pltpu.make_async_copy(dn_half(par), wd.at[me], loc.at[2])
    local_wout.start()
    local_up.start()
    local_dn.start()
    for dz in range(1, nz):
        @pl.when(z + dz >= nz)
        def _(dz=dz):
            up_first(dz).start()

    scale = hd ** (-0.5) * LOG2E

    def absorb(kv, gates, diagonal):
        for h in range(heads):
            cols = pl.ds(h * hd, hd)
            rel = (gates[h:h + 1, :] - gate_ref[h:h + 1, 0:1]) * LOG2E
            s = lax.dot_general(q_ref[:, cols], kv[:, cols], (((1,), (1,)), ((), ())),
                                preferred_element_type=jnp.float32)
            s = s * scale - rel
            if diagonal:
                qp = lax.broadcasted_iota(jnp.int32, s.shape, 0)
                kp = lax.broadcasted_iota(jnp.int32, s.shape, 1)
                s = jnp.where(kp <= qp, s, NEG)
            top = jnp.max(s, axis=1, keepdims=True)
            if not diagonal:
                old = m_s[:, h:h + 1]
                top = jnp.maximum(old, top)
                fade = jnp.exp2(old - top)
            w = jnp.exp2(s - top)
            total = jnp.sum(w, axis=1, keepdims=True)
            add = jnp.dot(w.astype(jnp.bfloat16), kv[:, pl.ds(width + h * hd, hd)],
                          preferred_element_type=jnp.float32)
            if not diagonal:
                total = l_s[:, h:h + 1] * fade + total
                add = acc_s[:, cols] * fade + add
            m_s[:, h:h + 1] = top
            l_s[:, h:h + 1] = total
            acc_s[:, cols] = add

    absorb(kv_ref, gate_ref, True)

    def level(i, carry):
        zs = z - i

        @pl.when(zs >= 0)
        def _():
            @pl.when(i > 0)
            def _():
                own = zs * ny + y
                rcopy(kv_ref, kv_all.at[own], kv_s1.at[0], kv_r.at[own], me).wait_recv()
                rcopy(gate_ref, gate_all.at[own], g_s1.at[0], g_r.at[own], me).wait_recv()

                @pl.when(z + 1 < nz)
                def _():
                    for c in kv_up(zs):
                        c.start()
                for dy in range(1, ny):
                    for c in kv_forward(zs, dy):
                        c.start()

            @pl.when(zs == 0)
            def _():
                for dz in range(1, nz):
                    @pl.when(z + dz < nz)
                    def _(dz=dz):
                        up_first(dz).start()
                for dy in range(1, ny):
                    up_own(dy).start()

            def column(dy, carry):
                s = zs * ny + (y + dy) % ny

                @pl.when(s < me)
                def _():
                    @pl.when(dy > 0)
                    def _():
                        rcopy(kv_ref, kv_all.at[s], kv_s1.at[0], kv_r.at[s], me).wait_recv()
                        rcopy(gate_ref, gate_all.at[s], g_s1.at[0], g_r.at[s], me).wait_recv()
                    absorb(kv_all.at[s], gate_all.at[s], False)
                return carry

            lax.fori_loop(0, ny, column, 0)
        return carry

    lax.fori_loop(0, nz, level, 0)

    for h in range(heads):
        cols = pl.ds(h * hd, hd)
        done = (acc_s[:, cols] / l_s[:, h:h + 1]).astype(jnp.bfloat16)
        for j in range(n_tp):
            att[j, :, cols] = done[j * rows:(j + 1) * rows, :]

    def heads_to(o):
        to = (tp + o) % n_tp
        return rcopy(att.at[to], att_in.at[tp], a_s.at[o], a_r.at[tp], me, to)

    for o in range(1, n_tp):
        heads_to(o).start()
    att_in[pl.ds(tp, 1)] = att[pl.ds(tp, 1)]
    local_wout.wait()
    for o in range(1, n_tp):
        src = (tp + o) % n_tp
        rcopy(att.at[0], att_in.at[src], a_s.at[0], a_r.at[src], me, tp).wait_recv()
    total = res_ref[...].astype(jnp.float32)
    for j in range(n_tp):
        total += jnp.dot(att_in[j], wout[j * width:(j + 1) * width, :], preferred_element_type=jnp.float32)
    rsum[...] = total
    mean_square = jnp.mean(total * total, axis=-1, keepdims=True)
    normed = (total * lax.rsqrt(mean_square + 1e-06) * gain_ref[...]).astype(jnp.bfloat16)

    chips = group // 2
    core = tp % 2
    mate = slot + 1 - 2 * core

    def block(ref, b):
        at = (b % 2) * chips + b // 2
        return ref.at[pl.ds(pl.multiple_of(at * rows, rows), rows), :]

    block(norm_all, slot)[...] = normed

    def normed_row(src, sem, other):
        zo, to = other // n_tp, other % n_tp
        return rcopy(block(norm_all, src), block(norm_all, src), n_s.at[sem], n_r.at[src],
                     (z - par + zo) * ny + y, to)

    def normed_chip(k):
        return normed_row(slot, k, (slot + 2 * k) % group)

    def normed_mate(k):
        return normed_row((slot + 2 * k) % group, chips + k, mate)

    for k in range(1, chips):
        normed_chip(k).start()
    normed_mate(0).start()
    for dz in range(1, nz):
        dn_first(dz).start()
    for dy in range(1, ny):
        dn_own(dy).start()

    for dz in range(1, nz):
        zs = (z - dz + nz) % nz
        s = zs * ny + y
        rcopy(up_half(0), wu_at(s), u_s1.at[0], u_r.at[s], me).wait_recv()
        for dy in range(1, ny):
            up_forward(zs, dy).start()
    for k in range(1, chips):
        src = (slot + 2 * k) % group
        rcopy(block(norm_all, src), block(norm_all, src), n_s.at[0], n_r.at[src], me).wait_recv()
        normed_mate(k).start()

    def down_on(dz):
        zs = (z - dz + nz) % nz
        s = zs * ny + y
        rcopy(dn_half(0), wd.at[s], d_s1.at[0], d_r.at[s], me).wait_recv()
        for dy in range(1, ny):
            dn_forward(zs, dy).start()

    local_up.wait()
    for dy in range(1, ny):
        for zs in range(nz):
            s = zs * ny + (y + dy) % ny
            rcopy(up_half(0), wu_at(s), u_s1.at[0], u_r.at[s], me).wait_recv()
    for k in range(chips):
        src = (mate + 2 * k) % group
        rcopy(block(norm_all, src), block(norm_all, src), n_s.at[0], n_r.at[src], me).wait_recv()

    tile = min(256, half)

    def up_tile(i, carry):
        cols = pl.ds(pl.multiple_of(i * tile, tile), tile)
        u = jnp.maximum(jnp.dot(norm_all[...], wu[:, cols], preferred_element_type=jnp.float32), 0.0)
        hid[:, cols] = (u * u).astype(jnp.bfloat16)
        return carry

    lax.fori_loop(0, half // tile, up_tile, 0)

    per = max(1, 128 // cs)
    span = ny * cs

    mine = slot // 2

    def part(ref, at, count, zs):
        return ref.at[pl.ds(pl.multiple_of(at * rows, rows), count * rows),
                      pl.ds(pl.multiple_of(zs * span, span), span)]

    def to_mate(zs):
        return rcopy(part(psend, (1 - core) * chips, chips, zs), part(pmate, 0, chips, zs),
                     q_s.at[zs], q_r.at[zs], me, mate % n_tp)

    def partial_to(k, zs):
        chip = (mine + k) % chips
        other = chip * 2 + core
        return rcopy(part(pcomb, chip, 1, zs), part(precv, mine, 1, zs), p_s.at[k * nz + zs],
                     p_r.at[mine * nz + zs], (z - par + other // n_tp) * ny + y, other % n_tp)

    def level_of(dz):
        return (z - dz + nz) % nz

    def down_level(dz):
        zs = level_of(dz)
        for k in range(ny // per):
            ws = [wd[zs * ny + k * per + i] for i in range(per)]
            w = ws[0] if per == 1 else jnp.concatenate(ws, axis=1)
            cols = pl.ds(pl.multiple_of((zs * ny + k * per) * cs, per * cs), per * cs)
            psend[:, cols] = jnp.dot(hid[...], w, preferred_element_type=jnp.float32).astype(jnp.bfloat16)
        to_mate(zs).start()

    def combine(dz):
        zs = level_of(dz)
        to_mate(zs).wait_recv()
        both = (part(psend, core * chips, chips, zs)[...].astype(jnp.float32)
                + part(pmate, 0, chips, zs)[...].astype(jnp.float32))
        part(pcomb, 0, chips, zs)[...] = both.astype(jnp.bfloat16)
        for k in range(1, chips):
            partial_to(k, zs).start()

    local_dn.wait()
    for dz in range(nz):
        if dz + 1 < nz:
            down_on(dz + 1)
        zs = (z - dz + nz) % nz
        for dy in range(1, ny):
            s = zs * ny + (y + dy) % ny
            rcopy(dn_half(0), wd.at[s], d_s1.at[0], d_r.at[s], me).wait_recv()
        down_level(dz)
        if dz > 0:
            combine(dz - 1)
    combine(nz - 1)

    total = rsum[...]
    whole_row = lambda ref, at: ref[pl.ds(pl.multiple_of(at * rows, rows), rows), :].astype(jnp.float32)
    total += whole_row(pcomb, mine)
    for k in range(1, chips):
        src = (mine + k) % chips
        for zs in range(nz):
            rcopy(part(pcomb, src, 1, zs), part(precv, src, 1, zs), p_s.at[0], p_r.at[src * nz + zs], me).wait_recv()
        total += whole_row(precv, src)
    out_ref[...] = total.astype(jnp.bfloat16)

    @pl.when(z + 1 < nz)
    def _():
        for c in kv_first():
            c.wait_send()
    for dz in range(1, nz):
        @pl.when((z + 1 < nz) & (z - dz >= 0))
        def _(dz=dz):
            for c in kv_up(z - dz):
                c.wait_send()
        up_first(dz).wait_send()
        dn_first(dz).wait_send()
    for dy in range(1, ny):
        @pl.when((y + dy) % ny > y)
        def _(dy=dy):
            for c in kv_own(dy):
                c.wait_send()
        up_own(dy).wait_send()
        dn_own(dy).wait_send()
        for dz in range(1, nz):
            zs = (z - dz + nz) % nz

            @pl.when(z - dz >= 0)
            def _(zs=zs, dy=dy):
                for c in kv_forward(zs, dy):
                    c.wait_send()
            up_forward(zs, dy).wait_send()
            dn_forward(zs, dy).wait_send()
    for o in range(1, n_tp):
        heads_to(o).wait_send()
    for k in range(1, chips):
        normed_chip(k).wait_send()
    for k in range(chips):
        normed_mate(k).wait_send()
    for zs in range(nz):
        to_mate(zs).wait_send()
        for k in range(1, chips):
            partial_to(k, zs).wait_send()


def per_device(n_sp, n_tp, queries, keys, values, cum_gate, residual, w_out, gain, w_up, w_down):
    tok, width = queries.shape
    heads = cum_gate.shape[1]
    rows, features = residual.shape
    ny = n_tp // 2
    nz = n_sp // ny
    group = 2 * n_tp
    half = w_up.shape[1] // 2
    bf, f32 = jnp.bfloat16, jnp.float32
    gates = jnp.pad(cum_gate.T, ((0, 8 - heads), (0, 0)))
    kv = jnp.concatenate([keys, values], axis=1)
    vmem = pl.BlockSpec(memory_space=pltpu.VMEM)
    hbm = pl.BlockSpec(memory_space=pl.ANY)
    dma = lambda n: pltpu.SemaphoreType.DMA((n,))
    return pl.pallas_call(
        functools.partial(body, n_sp, n_tp, heads),
        out_shape=jax.ShapeDtypeStruct((rows, features), bf),
        in_specs=[vmem, vmem, vmem, vmem, hbm, vmem, hbm, hbm],
        out_specs=vmem,
        scratch_shapes=[
            pltpu.VMEM((n_sp, tok, 2 * width), bf),
            pltpu.VMEM((n_sp,) + gates.shape, f32),
            pltpu.VMEM((tok, 128), f32),
            pltpu.VMEM((tok, 128), f32),
            pltpu.VMEM((tok, width), f32),
            pltpu.VMEM((n_tp, rows, width), bf),
            pltpu.VMEM((n_tp, rows, width), bf),
            pltpu.VMEM(w_out.shape, bf),
            pltpu.VMEM((rows, features), f32),
            pltpu.VMEM((n_sp * w_up.shape[0], half), bf),
            pltpu.VMEM((n_sp, half, w_down.shape[1]), bf),
            pltpu.VMEM((group * rows, features), bf),
            pltpu.VMEM((group * rows, half), bf),
            pltpu.VMEM((group * rows, features), bf),
            pltpu.VMEM((n_tp * rows, features), bf),
            pltpu.VMEM((n_tp * rows, features), bf),
            pltpu.VMEM((n_tp * rows, features), bf),
        ]
        + [dma(nz), dma(n_sp), dma(n_sp)] * 4
        + [dma(n_tp), dma(n_tp), dma(group), dma(group), dma(group * nz), dma(group * nz), dma(nz), dma(nz), dma(3)],
        compiler_params=pltpu.CompilerParams(
            collective_id=0, has_side_effects=True, vmem_limit_bytes=63 * 1024 * 1024
        ),
    )(queries, kv, gates, residual, w_out, gain.reshape(1, -1), w_up, w_down)


def solution(mesh):
    n_sp, n_tp = mesh.shape["sp"], mesh.shape["tp"]
    return jax.shard_map(
        functools.partial(per_device, n_sp, n_tp),
        mesh=mesh,
        in_specs=(
            P("sp", "tp"),
            P("sp", "tp"),
            P("sp", "tp"),
            P("sp", "tp"),
            P(("sp", "tp"), None),
            P(),
            P(),
            P("sp", "tp"),
            P("tp", "sp"),
        ),
        out_specs=P(("sp", "tp"), None),
        check_vma=False,
    )
```

```python
import functools
import math

import jax
import jax.numpy as jnp
from jax import lax
from jax.experimental import pallas as pl
from jax.experimental.pallas import tpu as pltpu
from jax.sharding import PartitionSpec as P

LOG2E = math.log2(math.e)
NEG = -1e30


def body(
    n_sp, n_tp, heads,
    q_ref, kv_ref, gate_ref, res_ref, wout_hbm, gain_ref, wup_hbm, wdn_hbm,
    out_ref,
    kv_all, gate_all, m_s, l_s, acc_s, att, att_in, wout, rsum,
    wu, wd, norm_all, hid, psend, pmate, pcomb, precv,
    kv_s1, kv_s2, kv_r, g_s1, g_s2, g_r, u_s1, u_s2, u_r, d_s1, d_s2, d_r,
    a_s, a_r, n_s, n_r, p_s, p_r, q_s, q_r, loc,
):
    ny = n_tp // 2
    nz = n_sp // ny
    tok, width = q_ref.shape
    hd = width // heads
    rows = tok // n_tp
    group = 2 * n_tp
    half = wu.shape[1]
    up_rows = wup_hbm.shape[0]
    features = res_ref.shape[1]
    cs = wdn_hbm.shape[1]
    me = lax.axis_index("sp")
    tp = lax.axis_index("tp")
    z, y = me // ny, me % ny
    par = z % 2
    slot = par * n_tp + tp

    def rcopy(src, dst, ss, rs, sp_to, tp_to=None):
        where = {"sp": sp_to} if tp_to is None else {"sp": sp_to, "tp": tp_to}
        return pltpu.make_async_remote_copy(
            src_ref=src, dst_ref=dst, send_sem=ss, recv_sem=rs,
            device_id=where, device_id_type=pl.DeviceIdType.MESH,
        )

    def member(o):
        other = (slot + o) % group
        return other, (z - par + other // n_tp) * ny + y, other % n_tp

    barrier = pltpu.get_barrier_semaphore()
    for dz in range(1, nz):
        pl.semaphore_signal(barrier, inc=1, device_id={"sp": ((z + dz) % nz) * ny + y},
                            device_id_type=pl.DeviceIdType.MESH)
    for dy in range(1, ny):
        pl.semaphore_signal(barrier, inc=1, device_id={"sp": z * ny + (y + dy) % ny},
                            device_id_type=pl.DeviceIdType.MESH)
    for o in range(1, group):
        _, sp_to, tp_to = member(o)
        pl.semaphore_signal(barrier, inc=1, device_id={"sp": sp_to, "tp": tp_to},
                            device_id_type=pl.DeviceIdType.MESH)
    pl.semaphore_wait(barrier, nz - 1 + ny - 1 + group - 1)

    def kv_up(zs):
        s = zs * ny + y
        to = me + ny
        return (rcopy(kv_all.at[s], kv_all.at[s], kv_s1.at[zs], kv_r.at[s], to),
                rcopy(gate_all.at[s], gate_all.at[s], g_s1.at[zs], g_r.at[s], to))

    def kv_first():
        to = me + ny
        return (rcopy(kv_ref, kv_all.at[me], kv_s1.at[z], kv_r.at[me], to),
                rcopy(gate_ref, gate_all.at[me], g_s1.at[z], g_r.at[me], to))

    def kv_own(dy):
        to = z * ny + (y + dy) % ny
        return (rcopy(kv_ref, kv_all.at[me], kv_s2.at[z * ny + dy], kv_r.at[me], to),
                rcopy(gate_ref, gate_all.at[me], g_s2.at[z * ny + dy], g_r.at[me], to))

    def kv_forward(zs, dy):
        s = zs * ny + y
        to = z * ny + (y + dy) % ny
        return (rcopy(kv_all.at[s], kv_all.at[s], kv_s2.at[zs * ny + dy], kv_r.at[s], to),
                rcopy(gate_all.at[s], gate_all.at[s], g_s2.at[zs * ny + dy], g_r.at[s], to))

    def wu_at(s):
        return wu.at[pl.ds(pl.multiple_of(s * up_rows, up_rows), up_rows), :]

    def up_half(p):
        return wup_hbm.at[:, pl.ds(pl.multiple_of(p * half, half), half)]

    def dn_half(p):
        return wdn_hbm.at[pl.ds(pl.multiple_of(p * half, half), half), :]

    def up_first(dz):
        zt = (z + dz) % nz
        return rcopy(up_half(zt % 2), wu_at(me), u_s1.at[dz], u_r.at[me], zt * ny + y)

    def dn_first(dz):
        zt = (z + dz) % nz
        return rcopy(dn_half(zt % 2), wd.at[me], d_s1.at[dz], d_r.at[me], zt * ny + y)

    def up_own(dy):
        return rcopy(up_half(par), wu_at(me), u_s2.at[z * ny + dy], u_r.at[me], z * ny + (y + dy) % ny)

    def dn_own(dy):
        return rcopy(dn_half(par), wd.at[me], d_s2.at[z * ny + dy], d_r.at[me], z * ny + (y + dy) % ny)

    def up_forward(zs, dy):
        s = zs * ny + y
        return rcopy(wu_at(s), wu_at(s), u_s2.at[zs * ny + dy], u_r.at[s], z * ny + (y + dy) % ny)

    def dn_forward(zs, dy):
        s = zs * ny + y
        return rcopy(wd.at[s], wd.at[s], d_s2.at[zs * ny + dy], d_r.at[s], z * ny + (y + dy) % ny)

    @pl.when(z + 1 < nz)
    def _():
        for c in kv_first():
            c.start()
    for dy in range(1, ny):
        @pl.when((y + dy) % ny > y)
        def _(dy=dy):
            for c in kv_own(dy):
                c.start()
    local_wout = pltpu.make_async_copy(wout_hbm, wout, loc.at[0])
    local_up = pltpu.make_async_copy(up_half(par), wu_at(me), loc.at[1])
    local_dn = pltpu.make_async_copy(dn_half(par), wd.at[me], loc.at[2])
    local_wout.start()
    local_up.start()
    local_dn.start()
    for dz in range(1, nz):
        @pl.when(z + dz >= nz)
        def _(dz=dz):
            up_first(dz).start()
    for dy in range(1, ny):
        up_own(dy).start()
    for dz in range(1, nz):
        @pl.when((z + dz >= nz) & (par == 0))
        def _(dz=dz):
            dn_first(dz).start()

    scale = hd ** (-0.5) * LOG2E

    def absorb(kv, gates, diagonal):
        for h in range(heads):
            cols = pl.ds(h * hd, hd)
            rel = (gates[h:h + 1, :] - gate_ref[h:h + 1, 0:1]) * LOG2E
            s = lax.dot_general(q_ref[:, cols], kv[:, cols], (((1,), (1,)), ((), ())),
                                preferred_element_type=jnp.float32)
            s = s * scale - rel
            if diagonal:
                qp = lax.broadcasted_iota(jnp.int32, s.shape, 0)
                kp = lax.broadcasted_iota(jnp.int32, s.shape, 1)
                s = jnp.where(kp <= qp, s, NEG)
            top = jnp.max(s, axis=1, keepdims=True)
            if not diagonal:
                old = m_s[:, h:h + 1]
                top = jnp.maximum(old, top)
                fade = jnp.exp2(old - top)
            w = jnp.exp2(s - top)
            total = jnp.sum(w, axis=1, keepdims=True)
            add = jnp.dot(w.astype(jnp.bfloat16), kv[:, pl.ds(width + h * hd, hd)],
                          preferred_element_type=jnp.float32)
            if not diagonal:
                total = l_s[:, h:h + 1] * fade + total
                add = acc_s[:, cols] * fade + add
            m_s[:, h:h + 1] = top
            l_s[:, h:h + 1] = total
            acc_s[:, cols] = add

    absorb(kv_ref, gate_ref, True)

    def level(i, carry):
        zs = z - i

        @pl.when(zs >= 0)
        def _():
            @pl.when(i > 0)
            def _():
                own = zs * ny + y
                rcopy(kv_ref, kv_all.at[own], kv_s1.at[0], kv_r.at[own], me).wait_recv()
                rcopy(gate_ref, gate_all.at[own], g_s1.at[0], g_r.at[own], me).wait_recv()

                @pl.when(z + 1 < nz)
                def _():
                    for c in kv_up(zs):
                        c.start()
                for dy in range(1, ny):
                    for c in kv_forward(zs, dy):
                        c.start()

            @pl.when(zs == 0)
            def _():
                for dz in range(1, nz):
                    @pl.when(z + dz < nz)
                    def _(dz=dz):
                        up_first(dz).start()
                for dz in range(1, nz):
                    @pl.when((z + dz < nz) & (par == 1))
                    def _(dz=dz):
                        dn_first(dz).start()

            def column(dy, carry):
                s = zs * ny + (y + dy) % ny

                @pl.when(s < me)
                def _():
                    @pl.when(dy > 0)
                    def _():
                        rcopy(kv_ref, kv_all.at[s], kv_s1.at[0], kv_r.at[s], me).wait_recv()
                        rcopy(gate_ref, gate_all.at[s], g_s1.at[0], g_r.at[s], me).wait_recv()
                    absorb(kv_all.at[s], gate_all.at[s], False)
                return carry

            lax.fori_loop(0, ny, column, 0)
        return carry

    lax.fori_loop(0, nz, level, 0)

    for h in range(heads):
        cols = pl.ds(h * hd, hd)
        done = (acc_s[:, cols] / l_s[:, h:h + 1]).astype(jnp.bfloat16)
        for j in range(n_tp):
            att[j, :, cols] = done[j * rows:(j + 1) * rows, :]

    def heads_to(o):
        to = (tp + o) % n_tp
        return rcopy(att.at[to], att_in.at[tp], a_s.at[o], a_r.at[tp], me, to)

    for o in range(1, n_tp):
        heads_to(o).start()
    for dz in range(1, nz):
        zs = (z - dz + nz) % nz
        s = zs * ny + y
        rcopy(up_half(0), wu_at(s), u_s1.at[0], u_r.at[s], me).wait_recv()
        for dy in range(1, ny):
            up_forward(zs, dy).start()
    for dy in range(1, ny):
        dn_own(dy).start()

    att_in[pl.ds(tp, 1)] = att[pl.ds(tp, 1)]
    local_wout.wait()
    for o in range(1, n_tp):
        src = (tp + o) % n_tp
        rcopy(att.at[0], att_in.at[src], a_s.at[0], a_r.at[src], me, tp).wait_recv()
    total = res_ref[...].astype(jnp.float32)
    for j in range(n_tp):
        total += jnp.dot(att_in[j], wout[j * width:(j + 1) * width, :], preferred_element_type=jnp.float32)
    rsum[...] = total
    mean_square = jnp.mean(total * total, axis=-1, keepdims=True)
    normed = (total * lax.rsqrt(mean_square + 1e-06) * gain_ref[...]).astype(jnp.bfloat16)

    chips = group // 2
    core = tp % 2
    mate = slot + 1 - 2 * core

    def block(ref, b):
        at = (b % 2) * chips + b // 2
        return ref.at[pl.ds(pl.multiple_of(at * rows, rows), rows), :]

    block(norm_all, slot)[...] = normed

    def normed_row(src, sem, other):
        zo, to = other // n_tp, other % n_tp
        return rcopy(block(norm_all, src), block(norm_all, src), n_s.at[sem], n_r.at[src],
                     (z - par + zo) * ny + y, to)

    def normed_chip(k):
        return normed_row(slot, k, (slot + 2 * k) % group)

    def normed_mate(k):
        return normed_row((slot + 2 * k) % group, chips + k, mate)

    for k in range(1, chips):
        normed_chip(k).start()
    normed_mate(0).start()
    for dz in range(1, nz):
        @pl.when((z + dz < nz) == (par == 0))
        def _(dz=dz):
            dn_first(dz).start()

    for k in range(1, chips):
        src = (slot + 2 * k) % group
        rcopy(block(norm_all, src), block(norm_all, src), n_s.at[0], n_r.at[src], me).wait_recv()
        normed_mate(k).start()

    def down_on(dz):
        zs = (z - dz + nz) % nz
        s = zs * ny + y
        rcopy(dn_half(0), wd.at[s], d_s1.at[0], d_r.at[s], me).wait_recv()
        for dy in range(1, ny):
            dn_forward(zs, dy).start()

    local_up.wait()
    for dy in range(1, ny):
        for zs in range(nz):
            s = zs * ny + (y + dy) % ny
            rcopy(up_half(0), wu_at(s), u_s1.at[0], u_r.at[s], me).wait_recv()
    for k in range(chips):
        src = (mate + 2 * k) % group
        rcopy(block(norm_all, src), block(norm_all, src), n_s.at[0], n_r.at[src], me).wait_recv()

    tile = min(256, half)

    def up_tile(i, carry):
        cols = pl.ds(pl.multiple_of(i * tile, tile), tile)
        u = jnp.maximum(jnp.dot(norm_all[...], wu[:, cols], preferred_element_type=jnp.float32), 0.0)
        hid[:, cols] = (u * u).astype(jnp.bfloat16)
        return carry

    lax.fori_loop(0, half // tile, up_tile, 0)

    per = max(1, 128 // cs)
    span = ny * cs

    mine = slot // 2

    def part(ref, at, count, zs):
        return ref.at[pl.ds(pl.multiple_of(at * rows, rows), count * rows),
                      pl.ds(pl.multiple_of(zs * span, span), span)]

    def to_mate(zs):
        return rcopy(part(psend, (1 - core) * chips, chips, zs), part(pmate, 0, chips, zs),
                     q_s.at[zs], q_r.at[zs], me, mate % n_tp)

    def partial_to(k, zs):
        chip = (mine + k) % chips
        other = chip * 2 + core
        return rcopy(part(pcomb, chip, 1, zs), part(precv, mine, 1, zs), p_s.at[k * nz + zs],
                     p_r.at[mine * nz + zs], (z - par + other // n_tp) * ny + y, other % n_tp)

    def level_of(dz):
        return (z - dz + nz) % nz

    def down_level(dz):
        zs = level_of(dz)
        for k in range(ny // per):
            ws = [wd[zs * ny + k * per + i] for i in range(per)]
            w = ws[0] if per == 1 else jnp.concatenate(ws, axis=1)
            cols = pl.ds(pl.multiple_of((zs * ny + k * per) * cs, per * cs), per * cs)
            psend[:, cols] = jnp.dot(hid[...], w, preferred_element_type=jnp.float32).astype(jnp.bfloat16)
        to_mate(zs).start()

    def combine(dz):
        zs = level_of(dz)
        to_mate(zs).wait_recv()
        both = (part(psend, core * chips, chips, zs)[...].astype(jnp.float32)
                + part(pmate, 0, chips, zs)[...].astype(jnp.float32))
        part(pcomb, 0, chips, zs)[...] = both.astype(jnp.bfloat16)
        for k in range(1, chips):
            partial_to(k, zs).start()

    local_dn.wait()
    for dz in range(nz):
        if dz + 1 < nz:
            down_on(dz + 1)
        zs = (z - dz + nz) % nz
        for dy in range(1, ny):
            s = zs * ny + (y + dy) % ny
            rcopy(dn_half(0), wd.at[s], d_s1.at[0], d_r.at[s], me).wait_recv()
        down_level(dz)
        if dz > 0:
            combine(dz - 1)
    combine(nz - 1)

    total = rsum[...]
    whole_row = lambda ref, at: ref[pl.ds(pl.multiple_of(at * rows, rows), rows), :].astype(jnp.float32)
    total += whole_row(pcomb, mine)
    for k in range(1, chips):
        src = (mine + k) % chips
        for zs in range(nz):
            rcopy(part(pcomb, src, 1, zs), part(precv, src, 1, zs), p_s.at[0], p_r.at[src * nz + zs], me).wait_recv()
        total += whole_row(precv, src)
    out_ref[...] = total.astype(jnp.bfloat16)

    @pl.when(z + 1 < nz)
    def _():
        for c in kv_first():
            c.wait_send()
    for dz in range(1, nz):
        @pl.when((z + 1 < nz) & (z - dz >= 0))
        def _(dz=dz):
            for c in kv_up(z - dz):
                c.wait_send()
        up_first(dz).wait_send()
        dn_first(dz).wait_send()
    for dy in range(1, ny):
        @pl.when((y + dy) % ny > y)
        def _(dy=dy):
            for c in kv_own(dy):
                c.wait_send()
        up_own(dy).wait_send()
        dn_own(dy).wait_send()
        for dz in range(1, nz):
            zs = (z - dz + nz) % nz

            @pl.when(z - dz >= 0)
            def _(zs=zs, dy=dy):
                for c in kv_forward(zs, dy):
                    c.wait_send()
            up_forward(zs, dy).wait_send()
            dn_forward(zs, dy).wait_send()
    for o in range(1, n_tp):
        heads_to(o).wait_send()
    for k in range(1, chips):
        normed_chip(k).wait_send()
    for k in range(chips):
        normed_mate(k).wait_send()
    for zs in range(nz):
        to_mate(zs).wait_send()
        for k in range(1, chips):
            partial_to(k, zs).wait_send()


def per_device(n_sp, n_tp, queries, keys, values, cum_gate, residual, w_out, gain, w_up, w_down):
    tok, width = queries.shape
    heads = cum_gate.shape[1]
    rows, features = residual.shape
    ny = n_tp // 2
    nz = n_sp // ny
    group = 2 * n_tp
    half = w_up.shape[1] // 2
    bf, f32 = jnp.bfloat16, jnp.float32
    gates = jnp.pad(cum_gate.T, ((0, 8 - heads), (0, 0)))
    kv = jnp.concatenate([keys, values], axis=1)
    vmem = pl.BlockSpec(memory_space=pltpu.VMEM)
    hbm = pl.BlockSpec(memory_space=pl.ANY)
    dma = lambda n: pltpu.SemaphoreType.DMA((n,))
    return pl.pallas_call(
        functools.partial(body, n_sp, n_tp, heads),
        out_shape=jax.ShapeDtypeStruct((rows, features), bf),
        in_specs=[vmem, vmem, vmem, vmem, hbm, vmem, hbm, hbm],
        out_specs=vmem,
        scratch_shapes=[
            pltpu.VMEM((n_sp, tok, 2 * width), bf),
            pltpu.VMEM((n_sp,) + gates.shape, f32),
            pltpu.VMEM((tok, 128), f32),
            pltpu.VMEM((tok, 128), f32),
            pltpu.VMEM((tok, width), f32),
            pltpu.VMEM((n_tp, rows, width), bf),
            pltpu.VMEM((n_tp, rows, width), bf),
            pltpu.VMEM(w_out.shape, bf),
            pltpu.VMEM((rows, features), f32),
            pltpu.VMEM((n_sp * w_up.shape[0], half), bf),
            pltpu.VMEM((n_sp, half, w_down.shape[1]), bf),
            pltpu.VMEM((group * rows, features), bf),
            pltpu.VMEM((group * rows, half), bf),
            pltpu.VMEM((group * rows, features), bf),
            pltpu.VMEM((n_tp * rows, features), bf),
            pltpu.VMEM((n_tp * rows, features), bf),
            pltpu.VMEM((n_tp * rows, features), bf),
        ]
        + [dma(nz), dma(n_sp), dma(n_sp)] * 4
        + [dma(n_tp), dma(n_tp), dma(group), dma(group), dma(group * nz), dma(group * nz), dma(nz), dma(nz), dma(3)],
        compiler_params=pltpu.CompilerParams(
            collective_id=0, has_side_effects=True, vmem_limit_bytes=63 * 1024 * 1024
        ),
    )(queries, kv, gates, residual, w_out, gain.reshape(1, -1), w_up, w_down)


def solution(mesh):
    n_sp, n_tp = mesh.shape["sp"], mesh.shape["tp"]
    return jax.shard_map(
        functools.partial(per_device, n_sp, n_tp),
        mesh=mesh,
        in_specs=(
            P("sp", "tp"),
            P("sp", "tp"),
            P("sp", "tp"),
            P("sp", "tp"),
            P(("sp", "tp"), None),
            P(),
            P(),
            P("sp", "tp"),
            P("tp", "sp"),
        ),
        out_specs=P(("sp", "tp"), None),
        check_vma=False,
    )
```
